32 devices in a mesh: sp: 8 (over z, y), tp: 4 (over x, core).
Axes of the slice: x: 2, y: 2, z: 4, core: 2. Of those that a mesh axis runs over, the one named last changes fastest.
Arguments:
- query: bfloat16 [12288, 512], P('sp', 'tp'), may hold values from -6 to 6
- key_rows: bfloat16 [12288, 512], P('sp', 'tp'), may hold values from -6 to 6
- value: bfloat16 [12288, 1024], P('sp', 'tp'), may hold values from -6 to 6
- in_gate: float32 [2, 8, 12288], P(None, 'tp', 'sp'), may hold values from -6 to 250
- forget_pre: float32 [2, 8, 12288], P(None, 'tp', 'sp'), may hold values from 0.3 to 12
- out_gate: bfloat16 [12288, 1024], P('sp', 'tp'), may hold values from -6 to 6
- head_gain: bfloat16 [1024], P('tp'), may hold values from 0.099609375 to 1.8984375
- out_weight: bfloat16 [1024, 2048], P('tp'), may hold values from -0.25 to 0.25
- stream: bfloat16 [12288, 2048], P('sp', 'tp'), may hold values from -16 to 16
- norm_gain: bfloat16 [2048], P('tp'), may hold values from 0.099609375 to 1.8984375
- gate_weight: bfloat16 [2048, 5632], P('sp', 'tp'), may hold values from -0.125 to 0.125
- up_weight: bfloat16 [2048, 5632], P('sp', 'tp'), may hold values from -0.125 to 0.125
- down_weight: bfloat16 [2048, 5632], P('sp', 'tp'), may hold values from -0.109375 to 0.109375
Outputs:
- layer_out: bfloat16 [12288, 2048], P('sp', 'tp')
The draws below stay inside these ranges and needn't reach their ends.
All inputs are finite; a program needn't handle non-finite values.
Results may differ from the reference program's by a relative error of at most 0.04.
Values may be sent and summed in bfloat16 or wider, within the bound.
A program may use at most 128 MiB of HBM per device.

```python
import jax
import jax.numpy as jnp
from jax import lax

D = 2048
MEMORY_HEADS = 8
DK = 64
DV = 128
FF = 5632
BLOCK = 128
TOK_DEV = 1536
SEQUENCE_TOKENS = 12288
N_TP = 4


def draw_in_gate(key, part):
    random_subkeys = jax.random.split(jax.random.fold_in(key, 11), 1)
    return jnp.clip(1.5 * jax.random.normal(random_subkeys[0], (2, MEMORY_HEADS, SEQUENCE_TOKENS), jnp.float32), -6.0, 6.0)


def draw_forget_pre(key, part):
    random_subkeys = jax.random.split(jax.random.fold_in(key, 23), 5)
    slow_share = 0.5
    slow = jax.random.uniform(random_subkeys[0], (2, MEMORY_HEADS, 1), jnp.float32) < slow_share
    spans = SEQUENCE_TOKENS // TOK_DEV
    factor = jnp.exp(jax.random.uniform(random_subkeys[1], (2, MEMORY_HEADS, spans), jnp.float32, -0.6931, 0.6931))
    factor = jnp.repeat(factor, TOK_DEV, axis=2)
    noise = 0.7 * jnp.clip(jax.random.normal(random_subkeys[2], (2, MEMORY_HEADS, SEQUENCE_TOKENS), jnp.float32), -2.5, 2.5)
    slow_pre = jnp.log(SEQUENCE_TOKENS / (0.6 * factor)) + noise
    fast_pre = jnp.log(50.0 / factor) + noise
    final_output = jnp.clip(jnp.where(slow, slow_pre, fast_pre), 0.3, 12.0)
    spike_list = jax.random.randint(random_subkeys[3], (2, MEMORY_HEADS, 3), 0, SEQUENCE_TOKENS)
    token_offset = jnp.arange(SEQUENCE_TOKENS)[None, None, None, :]
    flagged_entries = jnp.any(token_offset == spike_list[..., None], axis=2)
    spike_value = jax.random.uniform(random_subkeys[4], (2, MEMORY_HEADS, SEQUENCE_TOKENS), jnp.float32, 0.3, 1.5)
    return jnp.where(flagged_entries, spike_value, final_output)


def draw_stream(key, part):
    random_subkeys = jax.random.split(jax.random.fold_in(key, 37), 2)
    columns = jnp.arange(D, dtype=jnp.float32) / D
    rowdraw = jax.random.uniform(random_subkeys[1], (SEQUENCE_TOKENS, 1), jnp.float32)
    base = jnp.clip(jax.random.normal(random_subkeys[0], (SEQUENCE_TOKENS, D), jnp.float32), -4.0, 4.0)
    column_scale = jnp.exp(jnp.log(4.0) * (columns - 0.5))
    row_scale = jnp.exp(jnp.log(10.0) * (rowdraw - 0.7))
    return (base * row_scale * column_scale[None, :]).astype(jnp.bfloat16)


def raised(drawn, key, source, target, blocks, factor):
    def block_of(axis_at):
        return (jnp.arange(drawn.shape[axis_at]) // (drawn.shape[axis_at] // blocks)).reshape((-1,) + (1,) * (drawn.ndim - 1 - axis_at))

    first = jax.random.permutation(key, blocks)[block_of(target)]
    second = (block_of(target) + blocks // 2) % blocks
    return jnp.where((block_of(source) == first) | (block_of(source) == second), factor * drawn, drawn)


def block_scale(own_key, shape, cuts, least, largest):
    gain = 1.0
    for dim, blocks in cuts:
        draws = jax.random.uniform(jax.random.fold_in(jax.random.fold_in(own_key, 6), dim), (blocks,), jnp.float32, least / len(cuts), largest / len(cuts))
        gain = gain * jnp.repeat(jnp.exp(draws), shape[dim] // blocks).reshape((-1,) + (1,) * (len(shape) - 1 - dim))
    return gain


def scatter_about(rng, shape, scale, reach, cuts=(), kind=jnp.bfloat16):
    values = jax.random.normal(rng, shape, jnp.float32) * scale
    if len(cuts) > 0:
        values = block_scale(rng, shape, cuts, -0.22, 0.18) * values
    return jnp.clip(values, min=-reach, max=reach).astype(kind)


def gaussian_with(own_key, extent, spread, most, shards, heavy, held_as=jnp.bfloat16):
    values = spread * jax.random.normal(own_key, extent, jnp.float32)
    if shards:
        values = values * block_scale(own_key, extent, shards, -0.22, 0.18)
    return jnp.clip(raised(values, jax.random.fold_in(own_key, 3), *heavy), -most, most).astype(held_as)


def setup_inputs(seed: int = 0) -> dict:
    arg_keys = jax.random.split(jax.random.key(seed), 14)
    return {
        "query": scatter_about(arg_keys[0], (SEQUENCE_TOKENS, MEMORY_HEADS * DK), 1.0, 6.0, ((0, 8), (1, 4))),
        "key_rows": scatter_about(arg_keys[1], (SEQUENCE_TOKENS, MEMORY_HEADS * DK), 1.0, 6.0, ((0, 8), (1, 4))),
        "value": scatter_about(arg_keys[2], (SEQUENCE_TOKENS, MEMORY_HEADS * DV), 1.0, 6.0, ((0, 8), (1, 4))),
        "in_gate": draw_in_gate(jax.random.fold_in(arg_keys[13], 71), 0),
        "forget_pre": draw_forget_pre(jax.random.fold_in(arg_keys[13], 71), 0),
        "out_gate": scatter_about(arg_keys[5], (SEQUENCE_TOKENS, MEMORY_HEADS * DV), 1.5, 6.0, ((0, 8), (1, 4))),
        "head_gain": jnp.clip(1.0 + 0.18 * jax.random.normal(arg_keys[6], (MEMORY_HEADS * DV,), jnp.float32), 0.099609375, 1.8984375).astype(jnp.bfloat16),
        "out_weight": gaussian_with(arg_keys[7], (MEMORY_HEADS * DV, D), (MEMORY_HEADS * DV) ** -0.5, 0.25, ((0, 4),), (0, 1, 4, 2.0)),
        "stream": draw_stream(jax.random.fold_in(arg_keys[13], 71), 0),
        "norm_gain": jnp.clip(1.0 + 0.18 * jax.random.normal(arg_keys[9], (D,), jnp.float32), 0.099609375, 1.8984375).astype(jnp.bfloat16),
        "gate_weight": scatter_about(arg_keys[10], (D, FF), D ** -0.5, 0.125, ((0, 8), (1, 4))),
        "up_weight": scatter_about(arg_keys[11], (D, FF), D ** -0.5, 0.125, ((0, 8), (1, 4))),
        "down_weight": gaussian_with(arg_keys[12], (D, FF), FF ** -0.5, 0.109375, ((0, 8), (1, 4)), (1, 0, 8, 2.0)),
    }


HIGHEST = lax.Precision.HIGHEST
EPSILON = 1e-06

def direction(queries, keys, values, input_gates, forgets):
    head_count = queries.shape[0]
    block_count = queries.shape[1] // BLOCK

    def blocks(item):
        shaped = item.reshape((head_count, block_count, BLOCK) + item.shape[2:])
        return jnp.moveaxis(shaped, 1, 0)
    causal = jnp.tril(jnp.ones((BLOCK, BLOCK), dtype=bool))

    def step(carry, pieces):
        matrix, normer, stable = carry
        query_part, key_part, value_part, gate_part, forget_part = pieces
        cumulative = jnp.cumsum(forget_part, axis=-1)
        decay_log = jnp.where(causal, cumulative[:, :, None] - cumulative[:, None, :] + gate_part[:, None, :], -jnp.inf)
        carry_log = cumulative + stable[:, None]
        row_peak = jnp.maximum(carry_log, lax.optimization_barrier(jnp.max(decay_log, axis=-1)))
        scores = jnp.einsum('hjd,hsd->hjs', query_part, key_part, precision=HIGHEST) * jnp.exp(decay_log - row_peak[:, :, None])
        carried = jnp.exp(carry_log - row_peak)
        numerator = jnp.einsum('hjs,hsv->hjv', scores, value_part, precision=HIGHEST) + carried[:, :, None] * jnp.einsum('hvd,hjd->hjv', matrix, query_part, precision=HIGHEST)
        denominator = lax.optimization_barrier(jnp.sum(scores, axis=-1)) + carried * jnp.einsum('hd,hjd->hj', normer, query_part, precision=HIGHEST)
        output = numerator / jnp.maximum(jnp.abs(denominator), jnp.exp(-row_peak))[:, :, None]
        block_total = cumulative[:, -1]
        weight_log = block_total[:, None] - cumulative + gate_part
        new_stable = jnp.maximum(block_total + stable, lax.optimization_barrier(jnp.max(weight_log, axis=-1)))
        shrink = jnp.exp(block_total + stable - new_stable)
        weight = jnp.exp(weight_log - new_stable[:, None])
        new_matrix = shrink[:, None, None] * matrix + jnp.einsum('hsv,hsd->hvd', weight[:, :, None] * value_part, key_part, precision=HIGHEST)
        new_normer = shrink[:, None] * normer + jnp.einsum('hs,hsd->hd', weight, key_part, precision=HIGHEST)
        return ((new_matrix, new_normer, new_stable), output)
    initial = (jnp.zeros((head_count, values.shape[2], queries.shape[2]), jnp.float32), jnp.zeros((head_count, queries.shape[2]), jnp.float32), jnp.zeros((head_count,), jnp.float32))
    _, results = lax.scan(step, initial, (blocks(queries), blocks(keys), blocks(values), blocks(input_gates), blocks(forgets)))
    return jnp.moveaxis(results, 0, 1).reshape(head_count, -1, values.shape[2])

def reverse_time(item):
    return jnp.flip(item, axis=1)

def reference(query, key_rows, value, in_gate, forget_pre, out_gate, head_gain, out_weight, stream, norm_gain, gate_weight, up_weight, down_weight):
    length = query.shape[0]

    def split_heads(item, width):
        return jnp.transpose(item.astype(jnp.float32).reshape(length, MEMORY_HEADS, width), (1, 0, 2))
    queries = split_heads(query, DK) * DK ** (-0.5)
    keys = split_heads(key_rows, DK)
    values = split_heads(value, DV)
    gates_in = in_gate.astype(jnp.float32)
    forgets = jax.nn.log_sigmoid(forget_pre.astype(jnp.float32))
    forward = direction(queries, keys, values, gates_in[0], forgets[0])
    backward = reverse_time(direction(reverse_time(queries), reverse_time(keys), reverse_time(values), reverse_time(gates_in[1]), reverse_time(forgets[1])))
    summed = forward + backward
    head_normed = summed * lax.rsqrt(lax.optimization_barrier(jnp.mean(summed * summed, axis=-1, keepdims=True)) + EPSILON)
    merged = jnp.transpose(head_normed, (1, 0, 2)).reshape(length, MEMORY_HEADS * DV)
    gated = (merged * head_gain.astype(jnp.float32) * jax.nn.sigmoid(out_gate.astype(jnp.float32))).astype(jnp.bfloat16)
    group_width = MEMORY_HEADS * DV // N_TP
    mixed_sum = jnp.zeros((length, D), jnp.float32)
    for group_index in range(N_TP):
        lower = group_index * group_width
        partial_value = jnp.dot(gated[:, lower:lower + group_width], out_weight[lower:lower + group_width], preferred_element_type=jnp.float32)
        mixed_sum = mixed_sum + lax.optimization_barrier(partial_value.astype(jnp.bfloat16)).astype(jnp.float32)
    residual = stream.astype(jnp.float32) + mixed_sum
    normed = (residual * lax.rsqrt(lax.optimization_barrier(jnp.mean(residual * residual, axis=-1, keepdims=True)) + EPSILON) * norm_gain.astype(jnp.float32)).astype(jnp.bfloat16)
    hidden_width = FF // N_TP
    feed_sum = jnp.zeros((length, D), jnp.float32)
    for group_index in range(N_TP):
        lower = group_index * hidden_width
        gate_pre = jnp.dot(normed, gate_weight[:, lower:lower + hidden_width], preferred_element_type=jnp.float32)
        up_value = jnp.dot(normed, up_weight[:, lower:lower + hidden_width], preferred_element_type=jnp.float32)
        hidden = (jax.nn.silu(gate_pre) * up_value).astype(jnp.bfloat16)
        partial_value = jnp.dot(hidden, down_weight[:, lower:lower + hidden_width].T, preferred_element_type=jnp.float32)
        feed_sum = feed_sum + lax.optimization_barrier(partial_value.astype(jnp.bfloat16)).astype(jnp.float32)
    return (residual + feed_sum).astype(jnp.bfloat16)
```

```python
import functools

import jax
import jax.numpy as jnp
from jax import lax
from jax.experimental import pallas as pl
from jax.experimental.pallas import tpu as pltpu
from jax.sharding import PartitionSpec as P

BLOCK = 128
HIGHEST = lax.Precision.HIGHEST
EPSILON = 1e-06
VERY_LOW = -1e30


def two_pass(left, right, dims, split_left):
    wide = left if split_left else right
    high = wide.astype(jnp.bfloat16)
    low = (wide - high.astype(jnp.float32)).astype(jnp.bfloat16)
    total = None
    for part in (high, low):
        pair = (part, right) if split_left else (left, part)
        term = lax.dot_general(*pair, (dims, ((), ())), preferred_element_type=jnp.float32)
        total = term if total is None else total + term
    return total


def memory_kernel(
    heads,
    q_ref,
    k_ref,
    v_ref,
    col_ref,
    row_ref,
    c0_ref,
    n0_ref,
    m0_ref,
    og_ref,
    gain_ref,
    out_ref,
    c_ref,
    n_ref,
    m_ref,
    h_ref,
):
    blocks = row_ref.shape[0]
    units = 2 * heads
    depth_k = q_ref.shape[1] // heads
    depth_v = v_ref.shape[1] // heads
    c_ref[...] = c0_ref[...]
    n_ref[...] = n0_ref[...]
    m_ref[...] = m0_ref[...]
    at_row = lax.broadcasted_iota(jnp.int32, (BLOCK, BLOCK), 0)
    at_col = lax.broadcasted_iota(jnp.int32, (BLOCK, BLOCK), 1)
    lane = lax.broadcasted_iota(jnp.int32, (BLOCK, q_ref.shape[1]), 1)

    def step(index, carry):
        for direction in range(2):
            block = index if direction == 0 else blocks - 1 - index
            rows = pl.ds(pl.multiple_of(block * BLOCK, BLOCK), BLOCK)
            query = q_ref[rows, :].astype(jnp.float32) * depth_k ** (-0.5)
            key = k_ref[rows, :]
            key_wide = key.astype(jnp.float32)
            cols = col_ref[rows, :]
            row_block = row_ref[block]
            keep = at_col <= at_row if direction == 0 else at_col >= at_row
            for head in range(heads):
                unit = direction * heads + head
                mine = (lane >= head * depth_k) & (lane < (head + 1) * depth_k)
                q_wide = jnp.where(mine, query, 0.0)
                q_own = q_wide.astype(jnp.bfloat16)
                value = v_ref[rows, head * depth_v : (head + 1) * depth_v]
                b_col = cols[:, unit : unit + 1]
                a_col = cols[:, units + unit : units + unit + 1]
                a_row = row_block[unit : unit + 1, :]
                total = row_block[units + unit : units + unit + 1, :]
                m_row = m_ref[unit]
                n_row = n_ref[unit]
                c_state = c_ref[unit]
                decay = jnp.where(keep, b_col + a_row, VERY_LOW)
                carry_log = b_col + m_row[:, :1]
                peak = jnp.maximum(carry_log, jnp.max(decay, axis=1, keepdims=True))
                scores = lax.dot_general(
                    q_own, key, (((1,), (1,)), ((), ())), preferred_element_type=jnp.float32
                ) * jnp.exp(decay - peak)
                carried = jnp.exp(carry_log - peak)
                number = two_pass(scores, value, ((1,), (0,)), True)
                number = number + carried * two_pass(q_own, c_state, ((1,), (0,)), False)
                below = jnp.sum(scores, axis=1, keepdims=True)
                below = below + carried * jnp.sum(q_wide * n_row, axis=1, keepdims=True)
                h_ref[direction, rows, head * depth_v : (head + 1) * depth_v] = number / jnp.maximum(
                    jnp.abs(below), jnp.exp(-peak)
                )
                new_m = jnp.maximum(total + m_row, total + jnp.max(a_row, axis=1, keepdims=True))
                shrink = jnp.exp(total + m_row - new_m)
                weight = jnp.exp(total[:, :1] + a_col - new_m[:, :1])
                weighted = weight * value.astype(jnp.float32)
                c_ref[unit] = shrink[:, :1] * c_state + two_pass(
                    key, weighted, ((0,), (0,)), False
                )
                n_ref[unit] = shrink[:, :1] * n_row + jnp.sum(
                    weight * key_wide, axis=0, keepdims=True
                )
                m_ref[unit] = new_m
        return carry

    lax.fori_loop(0, blocks, step, 0)

    def finish(index, carry):
        rows = pl.ds(pl.multiple_of(index * BLOCK, BLOCK), BLOCK)
        for head in range(heads):
            span = slice(head * depth_v, (head + 1) * depth_v)
            summed = h_ref[0, rows, span] + h_ref[1, rows, span]
            scale = lax.rsqrt(jnp.mean(summed * summed, axis=1, keepdims=True) + EPSILON)
            opened = 1.0 / (1.0 + jnp.exp(-og_ref[rows, span].astype(jnp.float32)))
            out_ref[rows, span] = (
                summed * scale * gain_ref[:, span].astype(jnp.float32) * opened
            ).astype(jnp.bfloat16)
        return carry

    lax.fori_loop(0, blocks, finish, 0)


def swap(item, axis, distance):
    count = lax.axis_size(axis)
    return lax.ppermute(item, axis, [(j, j ^ distance) for j in range(count)])


def prior_state(own, slots, totals, peaks, matrices, normers):
    before = slots < own
    between = (slots[:, None] < slots[None, :]) & before[None, :]
    ahead = jnp.einsum(
        "kl,lh->kh", between.astype(jnp.float32), totals, precision=HIGHEST
    )
    span_total = jnp.sum(jnp.where(before[:, None], totals, 0.0), axis=0)
    log_weight = jnp.where(before[:, None], peaks + ahead, VERY_LOW)
    peak = jnp.maximum(span_total, jnp.max(log_weight, axis=0))
    weight = jnp.exp(log_weight - peak)
    matrix = jnp.sum(weight[:, :, None, None] * matrices, axis=0)
    normer = jnp.sum(weight[:, :, None] * normers, axis=0)
    return matrix, normer, peak


def scatter_sum(make, axis):
    count = lax.axis_size(axis)
    me = lax.axis_index(axis)
    half = count // 2
    far = [(me ^ 1) ^ (2 * j) for j in range(half)]
    near = [me ^ (2 * j) for j in range(half)]
    held = {}
    for j in range(half - 1, -1, -1):
        sent = swap(make(far[j]).astype(jnp.bfloat16), axis, 1)
        held[j] = make(near[j]) + sent.astype(jnp.float32)
    distance = half
    width = half
    while width > 1:
        width //= 2
        for j in range(width - 1, -1, -1):
            got = swap(held[j + width].astype(jnp.bfloat16), axis, 2 * width)
            held[j] = held[j] + got.astype(jnp.float32)
    return held[0]


def gather_features(item, axis):
    count = lax.axis_size(axis)
    pieces = [item]
    distance = count // 2
    while distance >= 1:
        pieces = pieces + [swap(p, axis, distance) for p in pieces]
        distance //= 2
    return pieces


def local(
    query,
    key_rows,
    value,
    in_gate,
    forget_pre,
    out_gate,
    head_gain,
    out_weight,
    stream,
    norm_gain,
    gate_weight,
    up_weight,
    down_weight,
):
    length = query.shape[0]
    heads = in_gate.shape[1]
    depth_k = query.shape[1] // heads
    depth_v = value.shape[1] // heads
    blocks = length // BLOCK
    n_sp = lax.axis_size("sp")
    n_tp = lax.axis_size("tp")
    sp = lax.axis_index("sp")
    tp = lax.axis_index("tp")
    width = stream.shape[1]
    features = width * n_tp
    hidden_width = gate_weight.shape[1]

    both = lax.all_gather(
        jnp.concatenate([gate_weight, up_weight], axis=1), "sp", axis=0, tiled=True
    )

    forgets = jax.nn.log_sigmoid(forget_pre).reshape(2, heads, blocks, BLOCK)
    gates = in_gate.reshape(2, heads, blocks, BLOCK)
    upper = jnp.triu(jnp.ones((BLOCK, BLOCK), jnp.float32))
    tri = jnp.stack([upper, upper.T])
    b = jnp.einsum("dhns,dsj->dhnj", forgets, tri, precision=HIGHEST)
    a = gates - b
    total = jnp.sum(forgets, axis=-1)
    grid_n = jnp.arange(blocks)
    later = (grid_n[:, None] < grid_n[None, :]).astype(jnp.float32)
    following = jnp.stack(
        [
            jnp.sum(total[0][:, None, :] * later[None], axis=-1),
            jnp.sum(total[1][:, None, :] * later.T[None], axis=-1),
        ]
    )
    own_log = (total + following)[..., None] + a
    own_peak = jnp.max(own_log, axis=(2, 3))
    own_total = jnp.sum(total, axis=-1)
    own_weight = jnp.exp(own_log - own_peak[..., None, None]).reshape(2 * heads, length)
    key_wide = key_rows.astype(jnp.float32)
    matrices = []
    for unit in range(2 * heads):
        head = unit % heads
        weighted = own_weight[unit][:, None] * value[:, head * depth_v : (head + 1) * depth_v].astype(
            jnp.float32
        )
        high = weighted.astype(jnp.bfloat16)
        matrices.append(
            lax.dot_general(
                key_rows, high, (((0,), (0,)), ((), ())), preferred_element_type=jnp.float32
            )[head * depth_k : (head + 1) * depth_k]
        )
    matrix = jnp.stack(matrices)
    normer_all = jnp.dot(own_weight, key_wide, precision=HIGHEST)
    normer = jnp.stack(
        [
            normer_all[u, (u % heads) * depth_k : (u % heads + 1) * depth_k]
            for u in range(2 * heads)
        ]
    )
    small = jnp.concatenate(
        [
            normer,
            own_peak.reshape(-1, 1),
            own_total.reshape(-1, 1),
            jnp.zeros((2 * heads, depth_v - depth_k - 2), jnp.float32),
        ],
        axis=1,
    )
    packed = jnp.concatenate([matrix, small[:, None, :], jnp.zeros((2 * heads, 7, depth_v), jnp.float32)], axis=1)
    others = jnp.stack([packed] + [swap(packed, "sp", k) for k in range(1, n_sp)])
    slots = sp ^ jnp.arange(n_sp)
    all_small = others[:, :, depth_k, :]
    states = []
    for direction in range(2):
        span = slice(direction * heads, (direction + 1) * heads)
        places, place = (slots, sp) if direction == 0 else (n_sp - 1 - slots, n_sp - 1 - sp)
        states.append(
            prior_state(
                place,
                places,
                all_small[:, span, depth_k + 1],
                all_small[:, span, depth_k],
                others[:, span, :depth_k, :],
                all_small[:, span, :depth_k],
            )
        )
    c0 = jnp.concatenate([s[0] for s in states], axis=0)
    n0 = jnp.concatenate([s[1] for s in states], axis=0)
    m0 = jnp.concatenate([s[2] for s in states], axis=0)

    def spread(item):
        placed = []
        for unit in range(2 * heads):
            head = unit % heads
            cut = item[unit]
            pads = [(head * depth_k, (heads - 1 - head) * depth_k)] + [(0, 0)] * (cut.ndim - 1)
            placed.append(jnp.pad(cut, pads))
        return jnp.stack(placed)

    c0 = spread(c0)
    n0 = spread(n0)[:, None, :]
    m0 = jnp.broadcast_to(m0[:, None, None], (2 * heads, 1, BLOCK))
    b_flat = b.reshape(2 * heads, length)
    a_flat = a.reshape(2 * heads, length)
    cols = jnp.concatenate([b_flat, a_flat], axis=0).T
    rows = jnp.concatenate(
        [
            a.reshape(2 * heads, blocks, BLOCK),
            jnp.broadcast_to(total.reshape(2 * heads, blocks, 1), (2 * heads, blocks, BLOCK)),
        ],
        axis=0,
    ).transpose(1, 0, 2)
    gated = pl.pallas_call(
        functools.partial(memory_kernel, heads),
        out_shape=jax.ShapeDtypeStruct((length, heads * depth_v), jnp.bfloat16),
        in_specs=[pl.BlockSpec(memory_space=pltpu.VMEM)] * 10,
        out_specs=pl.BlockSpec(memory_space=pltpu.VMEM),
        scratch_shapes=[
            pltpu.VMEM((2 * heads, heads * depth_k, depth_v), jnp.float32),
            pltpu.VMEM((2 * heads, 1, heads * depth_k), jnp.float32),
            pltpu.VMEM((2 * heads, 1, BLOCK), jnp.float32),
            pltpu.VMEM((2, length, heads * depth_v), jnp.float32),
        ],
        cost_estimate=pl.CostEstimate(
            flops=60 * length * 128 * 128 * 2, bytes_accessed=100_000_000, transcendentals=0
        ),
        name="memory",
    )(query, key_rows, value, cols, rows, c0, n0, m0, out_gate, head_gain[None, :])

    def mixed_part(index):
        cut = lax.dynamic_slice_in_dim(out_weight, index * width, width, axis=1)
        return jnp.dot(gated, cut, preferred_element_type=jnp.float32)

    residual = stream.astype(jnp.float32) + scatter_sum(mixed_part, "tp")
    squares = jnp.sum(residual * residual, axis=-1)
    scaled = (residual * norm_gain.astype(jnp.float32)).astype(jnp.bfloat16)
    pieces = gather_features(scaled, "tp")
    distances = [0]
    step = n_tp // 2
    while step >= 1:
        distances = distances + [d ^ step for d in distances]
        step //= 2
    square_total = sum(gather_features(squares.reshape(-1, BLOCK), "tp")).reshape(-1)
    row_scale = lax.rsqrt(square_total / features + EPSILON)[:, None]
    by_distance = {d: p for d, p in zip(distances, pieces)}

    ordered = [by_distance[d] for d in range(n_tp)]
    bit = 1
    while bit < n_tp:
        flip = (tp & bit) != 0
        ordered = [jnp.where(flip, ordered[d ^ bit], ordered[d]) for d in range(n_tp)]
        bit *= 2
    whole = jnp.concatenate(ordered, axis=1)

    down = lax.all_gather(down_weight, "sp", axis=0, tiled=True)
    gate_pre = jnp.dot(whole, both[:, :hidden_width], preferred_element_type=jnp.float32) * row_scale
    up_value = jnp.dot(whole, both[:, hidden_width:], preferred_element_type=jnp.float32) * row_scale
    hidden = (jax.nn.silu(gate_pre) * up_value).astype(jnp.bfloat16)

    def feed_piece(index):
        cut = lax.dynamic_slice_in_dim(down, index * width, width, axis=0)
        return lax.dot_general(
            hidden, cut, (((1,), (1,)), ((), ())), preferred_element_type=jnp.float32
        )

    return (residual + scatter_sum(feed_piece, "tp")).astype(jnp.bfloat16)


def solution(mesh):
    placed = (
        P("sp", "tp"),
        P("sp", "tp"),
        P("sp", "tp"),
        P(None, "tp", "sp"),
        P(None, "tp", "sp"),
        P("sp", "tp"),
        P("tp"),
        P("tp", None),
        P("sp", "tp"),
        P("tp"),
        P("sp", "tp"),
        P("sp", "tp"),
        P("sp", "tp"),
    )
    return jax.shard_map(
        local, mesh=mesh, in_specs=placed, out_specs=P("sp", "tp"), check_vma=False
    )
```
